256 devices in a mesh: kv: 64 (over z, y, core), tp: 4 (over x).
Axes of the slice: x: 4, y: 4, z: 8, core: 2. Of those that a mesh axis runs over, the one named last changes fastest.
Arguments:
- x_piece: bfloat16 [1024, 2048], P('kv'), may hold values from -6 to 6
- x_decode: bfloat16 [64, 2048], P('kv'), may hold values from -6 to 6
- norm_gain: float32 [2048], replicated, may hold values from 0.1 to 1.9
- w_query: bfloat16 [2048, 1024], P(None, 'tp'), may hold values from -0.1875 to 0.1875
- w_key: bfloat16 [2048, 1024], P(None, 'tp'), may hold values from -0.1875 to 0.1875
- w_value: bfloat16 [2048, 1024], P(None, 'tp'), may hold values from -0.125 to 0.125
- w_out: bfloat16 [1024, 2048], P(None, 'tp'), may hold values from -0.1875 to 0.1875
- head_gain: float32 [128], replicated, may hold values from 0.1 to 1.9
- lambdas: float32 [8], P('tp'), may hold values from 0.3 to 0.8
- piece_keys: bfloat16 [32768, 8, 128], P('kv', 'tp'), may hold values from -300 to 300
- piece_values: bfloat16 [32768, 8, 128], P('kv', 'tp'), may hold values from -6 to 6
- cache_keys: bfloat16 [64, 2048, 8, 128], P('kv', None, 'tp'), may hold values from -300 to 300
- cache_values: bfloat16 [64, 2048, 8, 128], P('kv', None, 'tp'), may hold values from -6 to 6
- cache_lengths: int32 [64], P('kv'), may hold values from 1 to 2048, as said below
Outputs:
- piece_out: bfloat16 [1024, 2048], P('kv', 'tp')
- decode_out: bfloat16 [64, 2048], P('kv', 'tp')
The draws below stay inside these ranges and needn't reach their ends.
Inputs may be any that keep to these rules, and one draw needn't show every extreme that they name: `cache_lengths`: some sequence has exactly 2048 filled slots.
All inputs are finite; a program needn't handle non-finite values.
Results may differ from the reference program's by a relative error of at most 0.013.
The reference program's roundings to bfloat16 on the way count: a program that leaves them out, or rounds other values in their place, can miss the bound.
Values may be sent and summed in bfloat16 or wider, within the bound.
A program may use at most 64 MiB of HBM per device.

```python
import jax
import jax.numpy as jnp
from jax import lax

D = 2048
HEADS = 8
DK = 64
DV = 128
DEC_LEN = 2048
PIECE = 1024
PAST = 32768
DEC = 64


def drawn_keys(key, shape):
    base = jax.random.normal(jax.random.fold_in(key, 11), shape, jnp.float32) * 1.32
    return jnp.clip(base, -300.0, 300.0).astype(jnp.bfloat16)


def draw_piece_keys(key, part):
    return drawn_keys(jax.random.fold_in(key, 21), (PAST, HEADS, 2 * DK))


def draw_cache_keys(key, part):
    return drawn_keys(jax.random.fold_in(key, 22), (DEC, DEC_LEN, HEADS, 2 * DK))


def draw_cache_lengths(key, part):
    first = jax.random.randint(jax.random.fold_in(key, 31), (DEC,), 1, DEC_LEN + 1)
    second = jax.random.randint(jax.random.fold_in(key, 32), (DEC,), 1, DEC_LEN + 1)
    lengths = jnp.minimum(first, second)
    longest = jax.random.randint(jax.random.fold_in(key, 33), (), 0, DEC)
    return lengths.at[longest].set(DEC_LEN).astype(jnp.int32)


def shard_levels(key, shape, pieces, low, largest):
    factor_of = 1.0
    for dim, blocks in pieces:
        draws = jax.random.uniform(jax.random.fold_in(jax.random.fold_in(key, 6), dim), (blocks,), jnp.float32, low / len(pieces), largest / len(pieces))
        factor_of = factor_of * jnp.repeat(jnp.exp(draws), shape[dim] // blocks).reshape((-1,) + (1,) * (len(shape) - 1 - dim))
    return factor_of


def normal_values(own_key, dims, width, limit, pieces=(), held_as=jnp.bfloat16):
    factor_of = shard_levels(own_key, dims, pieces, -0.22, 0.18) if pieces else 1.0
    entries = jax.random.normal(own_key, dims, jnp.float32) * width * factor_of
    return jnp.minimum(jnp.maximum(entries, -limit), limit).astype(held_as)


def setup_inputs(seed: int = 0) -> dict:
    splits = jax.random.split(jax.random.key(seed), 15)
    return {
        "x_piece": normal_values(splits[0], (PIECE, D), 1.0, 6.0, ((0, 64),)),
        "x_decode": normal_values(splits[1], (DEC, D), 1.0, 6.0, ((0, 64),)),
        "norm_gain": jnp.clip(1.0 + 0.18 * jax.random.normal(splits[2], (D,), jnp.float32), 0.1, 1.9),
        "w_query": normal_values(splits[3], (D, HEADS * 2 * DK), (4 * D // 7) ** -0.5, 0.1875, ((1, 4),)),
        "w_key": normal_values(splits[4], (D, HEADS * 2 * DK), (4 * D // 7) ** -0.5, 0.1875, ((1, 4),)),
        "w_value": normal_values(splits[5], (D, HEADS * DV), D ** -0.5, 0.125, ((1, 4),)),
        "w_out": normal_values(splits[6], (HEADS * DV, D), (HEADS * DV) ** -0.5, 0.1875, ((1, 4),)),
        "head_gain": jnp.clip(1.0 + 0.18 * jax.random.normal(splits[7], (DV,), jnp.float32), 0.1, 1.9),
        "lambdas": jnp.clip(0.3 + 0.5 * jax.random.uniform(splits[8], (HEADS,), jnp.float32) ** shard_levels(splits[8], (HEADS,), ((0, 4),), -0.2, 0.2), 0.3, 0.8),
        "piece_keys": draw_piece_keys(jax.random.fold_in(splits[14], 71), 0),
        "piece_values": normal_values(splits[10], (PAST, HEADS, DV), 1.0, 6.0, ((0, 64), (1, 4))),
        "cache_keys": draw_cache_keys(jax.random.fold_in(splits[14], 71), 0),
        "cache_values": normal_values(splits[12], (DEC, DEC_LEN, HEADS, DV), 1.0, 6.0, ((0, 64), (2, 4))),
        "cache_lengths": draw_cache_lengths(jax.random.fold_in(splits[14], 71), 0),
    }


EPS = 1e-06

def project_rows(rows, norm_gain, w_query, w_key, w_value):
    values32 = rows.astype(jnp.float32)
    normed = (values32 * lax.rsqrt(lax.optimization_barrier(jnp.mean(values32 * values32, axis=-1, keepdims=True)) + EPS) * norm_gain).astype(jnp.bfloat16)
    count = rows.shape[0]
    queries = jnp.dot(normed, w_query, preferred_element_type=jnp.float32).astype(jnp.bfloat16).reshape(count, HEADS, 2 * DK)
    new_keys = jnp.dot(normed, w_key, preferred_element_type=jnp.float32).astype(jnp.bfloat16).reshape(count, HEADS, 2 * DK)
    new_values = jnp.dot(normed, w_value, preferred_element_type=jnp.float32).astype(jnp.bfloat16).reshape(count, HEADS, DV)
    return (queries, new_keys, new_values)

def head_norm(attended, head_gain):
    return (attended * lax.rsqrt(lax.optimization_barrier(jnp.mean(attended * attended, axis=-1, keepdims=True)) + EPS) * head_gain).astype(jnp.bfloat16)

def reference(x_piece, x_decode, norm_gain, w_query, w_key, w_value, w_out, head_gain, lambdas, piece_keys, piece_values, cache_keys, cache_values, cache_lengths):
    score_scale = 1.0 / DK ** 0.5
    piece_q, piece_k, piece_v = project_rows(x_piece, norm_gain, w_query, w_key, w_value)
    dec_q, dec_k, dec_v = project_rows(x_decode, norm_gain, w_query, w_key, w_value)
    keys_all = jnp.concatenate([piece_keys, piece_k], axis=0).transpose(1, 0, 2)
    values_all = jnp.concatenate([piece_values, piece_v], axis=0).transpose(1, 0, 2)
    key_index = jnp.arange(PAST + PIECE, dtype=jnp.int32)
    block_rows = 512 if PIECE % 512 == 0 else PIECE
    nblocks = PIECE // block_rows

    def one_head(inputs):
        head_q, head_k, head_v, weight_two = inputs
        blocks = head_q.reshape(nblocks, block_rows, 2 * DK)

        def one_block(binputs):
            query_block, block_start = binputs
            query_pos = block_start + jnp.arange(block_rows, dtype=jnp.int32)
            allowed = (key_index[None, :] < PAST) | (key_index[None, :] - PAST <= query_pos[:, None])
            results = []
            for which_map in range(2):
                lower = which_map * DK
                scores = jnp.dot(query_block[:, lower:lower + DK], head_k[:, lower:lower + DK].T, preferred_element_type=jnp.float32) * score_scale
                scores = jnp.where(allowed, scores, -jnp.inf)
                row_max = lax.optimization_barrier(jnp.max(scores, axis=-1, keepdims=True))
                weights = jnp.exp(scores - row_max)
                totals = lax.optimization_barrier(jnp.sum(weights, axis=-1, keepdims=True))
                mixed = jnp.dot(weights.astype(jnp.bfloat16), head_v, preferred_element_type=jnp.float32)
                results.append(mixed / totals)
            return results[0] - weight_two * results[1]
        starts = jnp.arange(nblocks, dtype=jnp.int32) * block_rows
        return lax.map(one_block, (blocks, starts)).reshape(PIECE, DV)
    piece_att = lax.map(one_head, (piece_q.transpose(1, 0, 2), keys_all, values_all, lambdas))
    piece_att = piece_att.transpose(1, 0, 2)
    slot_index = jnp.arange(DEC_LEN + 1, dtype=jnp.int32)

    def one_sequence(inputs):
        seq_q, seq_k, seq_v, own_k, own_v, length = inputs
        keys = jnp.concatenate([seq_k, own_k[None]], axis=0).astype(jnp.float32)
        values = jnp.concatenate([seq_v, own_v[None]], axis=0).astype(jnp.float32)
        allowed = (slot_index < length) | (slot_index == DEC_LEN)
        query32 = seq_q.astype(jnp.float32)
        results = []
        for which_map in range(2):
            lower = which_map * DK
            scores = jnp.einsum('hd,khd->hk', query32[:, lower:lower + DK], keys[:, :, lower:lower + DK]) * score_scale
            scores = jnp.where(allowed[None, :], scores, -jnp.inf)
            row_max = lax.optimization_barrier(jnp.max(scores, axis=-1, keepdims=True))
            weights = jnp.exp(scores - row_max)
            totals = lax.optimization_barrier(jnp.sum(weights, axis=-1, keepdims=True))
            mixed = jnp.einsum('hk,khd->hd', weights.astype(jnp.bfloat16).astype(jnp.float32), values)
            results.append(mixed / totals)
        return results[0] - lambdas[:, None] * results[1]
    dec_att = lax.map(one_sequence, (dec_q, cache_keys, cache_values, dec_k, dec_v, cache_lengths))
    piece_heads = head_norm(piece_att, head_gain).reshape(PIECE, HEADS * DV)
    dec_heads = head_norm(dec_att, head_gain).reshape(DEC, HEADS * DV)
    piece_out = jnp.dot(piece_heads, w_out, preferred_element_type=jnp.float32).astype(jnp.bfloat16)
    decode_out = jnp.dot(dec_heads, w_out, preferred_element_type=jnp.float32).astype(jnp.bfloat16)
    return (piece_out, decode_out)
```

```python
import functools

import jax
import jax.numpy as jnp
from jax import lax
from jax.experimental import pallas as pl
from jax.experimental.pallas import tpu as pltpu
from jax.sharding import PartitionSpec as P

EPS = 1e-06
MESH = pl.DeviceIdType.MESH
NT = (((1,), (1,)), ((), ()))
LAG = 1


def kernel(
    Z, Y, X,
    x_hbm, xd_hbm, gain_hbm, wq_hbm, wk_hbm, wv_hbm, wo_hbm, hg_hbm, lam, pk_hbm, pv_hbm,
    ck_hbm, cv_hbm, length,
    out_p, out_d,
    x_v, xd_v, gain_v, hg_v, w_v, wo_v, kraw, vraw, kd, vd, ck_v, cv_v, tmp,
    nkv, nkv_in, qbuf, ysend, ysst, yrecv, yrst, zsend, zsst, zrecv, zrst, hbuf, dbuf,
    lsem, ps, pr, qzs, qzr, qys, qyr, yds, ydr, yss, ysr, zds, zdr, zss, zsr, hs, hr, ds, dr,
):
    kv = lax.axis_index("kv")
    tp = lax.axis_index("tp")
    core = lax.rem(kv, 2)
    chip = lax.div(kv, 2)
    y = lax.rem(chip, Y)
    z = lax.div(chip, Y)
    rows = x_v.shape[0]
    npos = kraw.shape[1] // 2
    pairs = Z // 2

    def dev(zz, yy):
        return ((zz * Y + yy) * 2 + core, tp)

    partner = (chip * 2 + 1 - core, tp)

    def xdev(xx):
        return (kv, xx)

    def mod(a, n):
        return lax.rem(a + n, n)

    barrier = pltpu.get_barrier_semaphore()
    for d in range(1, Z):
        pl.semaphore_signal(barrier, inc=1, device_id=dev(mod(z + d, Z), y), device_id_type=MESH)
    for d in range(1, Y):
        pl.semaphore_signal(barrier, inc=1, device_id=dev(z, mod(y + d, Y)), device_id_type=MESH)
    for d in range(1, X):
        pl.semaphore_signal(barrier, inc=1, device_id=xdev(mod(tp + d, X)), device_id_type=MESH)
    pl.semaphore_signal(barrier, inc=1, device_id=partner, device_id_type=MESH)

    local = []

    def fetch(src, dst):
        copy = pltpu.make_async_copy(src, dst, lsem.at[len(local)])
        copy.start()
        local.append(copy)
        return copy

    c_x = fetch(x_hbm, x_v)
    c_xd = fetch(xd_hbm, xd_v)
    c_gain = fetch(gain_hbm, gain_v)
    c_wq = fetch(wq_hbm, w_v.at[0])
    c_wk = fetch(wk_hbm, w_v.at[1])
    c_wv = fetch(wv_hbm, w_v.at[2])
    c_pk = fetch(pk_hbm, kraw.at[0])
    c_pv = fetch(pv_hbm, vraw.at[0])
    c_ck = fetch(ck_hbm, ck_v)
    c_cv = fetch(cv_hbm, cv_v)
    c_wo = fetch(wo_hbm, wo_v)
    c_hg = fetch(hg_hbm, hg_v)

    def remote(src, dst, ssem, rsem, device):
        return pltpu.make_async_remote_copy(
            src_ref=src, dst_ref=dst, send_sem=ssem, recv_sem=rsem,
            device_id=device, device_id_type=MESH,
        )

    c_x.wait()
    c_xd.wait()
    c_gain.wait()
    gain = gain_v[...]

    def norm(v):
        v = v.astype(jnp.float32)
        return v * lax.rsqrt(jnp.mean(v * v, axis=-1, keepdims=True) + EPS) * gain

    normed_p = norm(x_v[...]).astype(jnp.bfloat16)
    normed_d = jnp.broadcast_to(norm(xd_v[...]), (16, x_v.shape[1])).astype(jnp.bfloat16)
    normed = jnp.concatenate([normed_p, normed_d], axis=0)

    def project(which):
        return jnp.dot(normed, w_v[which], preferred_element_type=jnp.float32).astype(jnp.bfloat16)

    c_wq.wait()
    queries = project(0) * jnp.bfloat16(0.125)
    qbuf[z, y] = queries[:rows]

    pl.semaphore_wait(barrier, Z + Y + X - 2)

    def q_z(d):
        return remote(qbuf.at[z, y], qbuf.at[z, y], qzs.at[d], qzr.at[d], dev(mod(z + d, Z), y))

    def q_z_in(d):
        src = mod(z + Z - d, Z)
        return remote(qbuf.at[src, y], qbuf.at[src, y], qzs.at[d], qzr.at[d], dev(src, y))

    def q_y(o, e):
        zz = mod(z + o, Z)
        return remote(
            qbuf.at[zz, y], qbuf.at[zz, y], qys.at[o, e], qyr.at[o, e], dev(z, mod(y + e, Y))
        )

    def q_y_in(o, e):
        zz = mod(z + o, Z)
        src = mod(y + Y - e, Y)
        return remote(qbuf.at[zz, src], qbuf.at[zz, src], qys.at[o, e], qyr.at[o, e], dev(z, src))

    zorder = []
    for d in range(1, Z // 2 + 1):
        zorder.append(d)
        if Z - d not in zorder:
            zorder.append(Z - d)
    for d in reversed(zorder):
        q_z(d).start()
    for e in range(1, Y):
        q_y(0, e).start()

    p_k = remote(pk_hbm, kraw.at[1], ps.at[0], pr.at[0], partner)
    p_v = remote(pv_hbm, vraw.at[1], ps.at[1], pr.at[1], partner)
    p_n = remote(nkv, nkv_in, ps.at[2], pr.at[2], partner)
    p_k.start()
    p_v.start()

    c_wk.wait()
    keys = project(1)
    c_wv.wait()
    values = project(2)
    nkv[...] = jnp.concatenate([keys[:rows], values[:rows]], axis=1)
    p_n.start()

    def forward(d):
        q_z_in(d).wait_recv()
        for e in range(1, Y):
            q_y(Z - d, e).start()

    def split_heads(raw, which, out):
        tmp[...] = raw[which].astype(jnp.float32)
        for h in range(2):
            out[h, pl.ds(which * npos, npos), :] = tmp[
                pl.ds(h, npos, stride=2), :
            ].astype(jnp.bfloat16)

    c_pk.wait()
    split_heads(kraw, 0, kd)
    c_pv.wait()
    split_heads(vraw, 0, vd)

    for d in zorder[:2]:
        forward(d)

    c_ck.wait()
    c_cv.wait()
    c_hg.wait()
    head_gain = hg_v[...]
    row_id = lax.broadcasted_iota(jnp.int32, (16, 128), 0)
    lane_id = lax.broadcasted_iota(jnp.int32, (16, 128), 1)
    first_head = (row_id & 3) < 2
    own_half = (lane_id >= 64) == ((row_id & 1) == 1)

    def by_head(m):
        m = m[rows:].astype(jnp.float32)
        return jnp.where(first_head, m[:, :128], m[:, 128:])

    dq = jnp.where(own_half, by_head(queries), 0.0)
    own_score = jnp.sum(dq * by_head(keys), axis=-1, keepdims=True)
    scores = lax.dot_general(
        dq.astype(jnp.bfloat16), ck_v[...], NT, preferred_element_type=jnp.float32
    )
    slots = scores.shape[1]
    s_row = lax.broadcasted_iota(jnp.int32, (16, slots), 0)
    s_col = lax.broadcasted_iota(jnp.int32, (16, slots), 1)
    head_ok = (s_col & 1) == ((s_row >> 1) & 1)
    scores = jnp.where(head_ok & (s_col < 2 * length[0]), scores, -jnp.inf)
    d_max = jnp.maximum(jnp.max(scores, axis=-1, keepdims=True), own_score)
    weights = jnp.exp(scores - d_max)
    own_weight = jnp.exp(own_score - d_max)
    d_tot = jnp.sum(weights, axis=-1, keepdims=True) + own_weight
    mixed = jnp.dot(weights.astype(jnp.bfloat16), cv_v[...], preferred_element_type=jnp.float32)
    mixed = mixed + own_weight.astype(jnp.bfloat16).astype(jnp.float32) * by_head(values)
    mixed = mixed / d_tot

    def head_norm(a):
        return a * lax.rsqrt(jnp.mean(a * a, axis=-1, keepdims=True) + EPS) * head_gain

    d_heads = []
    for h in range(2):
        att = mixed[2 * h : 2 * h + 1] - lam[h] * mixed[2 * h + 1 : 2 * h + 2]
        d_heads.append(jnp.broadcast_to(head_norm(att), (16, 128)))
    dbuf[0] = jnp.concatenate(d_heads, axis=1).astype(jnp.bfloat16)

    def h_copy(buf, ss, rs, d):
        return remote(buf.at[0], buf.at[d], ss.at[d], rs.at[d], xdev(mod(tp + d, X)))

    for d in range(1, X):
        h_copy(dbuf, ds, dr, d).start()

    for d in zorder[2:]:
        forward(d)

    zeros = jnp.zeros((96, 128), jnp.bfloat16)
    p_n.wait_recv()
    for h in range(2):
        for out, base in ((kd, 0), (vd, 256)):
            cols = slice(base + h * 128, base + (h + 1) * 128)
            out[h, 2 * npos : 2 * npos + 16, :] = nkv[:, cols]
            out[h, 2 * npos + 16 : 2 * npos + 32, :] = nkv_in[:, cols]
            out[h, 2 * npos + 32 :, :] = zeros
    p_k.wait_recv()
    split_heads(kraw, 1, kd)
    p_v.wait_recv()
    split_heads(vraw, 1, vd)

    block = Y * 16
    st_lane = lax.broadcasted_iota(jnp.int32, (8, 128), 1)
    q_row = lax.broadcasted_iota(jnp.int32, (4 * block, 128), 0)
    q_lane = lax.broadcasted_iota(jnp.int32, (4 * block, 128), 1)
    in_pair = lax.rem(q_row, 2 * block)
    second = in_pair >= block
    in_block = lax.rem(in_pair, block)
    q_y_of = lax.div(in_block, 16)
    q_i = lax.rem(in_block, 16)
    key_core = jnp.where(q_lane < 16, core, 1 - core)
    key_pos = chip * 32 + key_core * 16 + lax.rem(q_lane, 16)

    def offsets(k):
        return lax.rem(Z - k, Z), k + 1

    def y_copies(k, d):
        to = mod(y + d, Y)
        who = dev(z, to)
        return (
            remote(ysend.at[k, to], yrecv.at[k, d], yds.at[k, d], ydr.at[k, d], who),
            remote(ysst.at[k, to], yrst.at[k, d], yss.at[k, d], ysr.at[k, d], who),
        )

    def chunk(k):
        oa, ob = offsets(k)
        za, zb = mod(z + oa, Z), mod(z + ob, Z)
        for e in range(1, Y):
            q_y_in(oa, e).wait_recv()
            q_y_in(ob, e).wait_recv()
        q = jnp.concatenate(
            [qbuf[za].reshape(block, 256), qbuf[zb].reshape(block, 256)], axis=0
        )
        z_of = jnp.where(second, zb, za)
        q_pos = (z_of * Y + q_y_of) * 32 + core * 16 + q_i
        visible = (key_pos <= q_pos) & (q_lane < 32)
        lane2 = lax.broadcasted_iota(jnp.int32, (2 * block, 128), 1)
        stats = [jnp.zeros((8, 128), jnp.float32) for _ in range(Y)]
        for h in range(2):
            qh = q[:, h * 128 : (h + 1) * 128]
            zero = jnp.zeros_like(qh)
            stacked = jnp.concatenate(
                [jnp.where(lane2 < 64, qh, zero), jnp.where(lane2 < 64, zero, qh)], axis=0
            )
            s = lax.dot_general(stacked, kd[h], NT, preferred_element_type=jnp.float32)
            s = jnp.concatenate(
                [s[:, : 2 * npos], jnp.where(visible, s[:, 2 * npos :], -jnp.inf)], axis=1
            )
            top = jnp.max(s, axis=-1, keepdims=True)
            w = jnp.exp(s - top)
            tot = jnp.sum(w, axis=-1, keepdims=True)
            acc = jnp.dot(
                w.astype(jnp.bfloat16), vd[h], preferred_element_type=jnp.float32
            ).astype(jnp.bfloat16)
            for m in range(2):
                combo = 2 * h + m
                for zi in range(2):
                    for yy in range(Y):
                        base = m * 2 * block + zi * block + yy * 16
                        ysend[k, yy, zi * 16 : zi * 16 + 16, combo * 128 : (combo + 1) * 128] = (
                            acc[base : base + 16]
                        )
                        for half in range(2):
                            lane = zi * 8 + half * 4 + combo
                            r0 = base + half * 8
                            stats[yy] = jnp.where(st_lane == lane, top[r0 : r0 + 8], stats[yy])
                            stats[yy] = jnp.where(
                                st_lane == lane + 64, tot[r0 : r0 + 8], stats[yy]
                            )
        for yy in range(Y):
            ysst[k, yy] = stats[yy]
        for d in range(1, Y):
            for copy in y_copies(k, d):
                copy.start()

    def merged(stats, blocks, zi):
        top = functools.reduce(jnp.maximum, stats)
        scale = [jnp.exp(s - top) for s in stats]
        total = sum(pltpu.roll(f, 64, 1) * s for f, s in zip(scale, stats))
        outs = []
        for combo in range(4):
            lane = zi * 8 + combo
            acc = None
            for f, b in zip(scale, blocks):
                col = jnp.concatenate([f[:, lane : lane + 1], f[:, lane + 4 : lane + 5]], axis=0)
                term = col * b(combo)
                acc = term if acc is None else acc + term
            outs.append(acc)
        return top, total, outs

    def z_copies(k, zi):
        o = offsets(k)[zi]
        who = dev(mod(z + o, Z), y)
        return (
            remote(zsend.at[k, zi], zrecv.at[k, zi], zds.at[k, zi], zdr.at[k, zi], who),
            remote(zsst.at[k], zrst.at[k, zi], zss.at[k, zi], zsr.at[k, zi], who),
        )

    def combine(k):
        for d in range(1, Y):
            for copy in y_copies(k, d):
                copy.wait_recv()
        stats = [ysst[k, y]] + [yrst[k, d] for d in range(1, Y)]
        for zi in range(2):
            blocks = []
            for d in range(Y):
                src = ysend[k, y, zi * 16 : zi * 16 + 16, :] if d == 0 else yrecv[
                    k, d, zi * 16 : zi * 16 + 16, :
                ]
                blocks.append(
                    lambda c, src=src: src[:, c * 128 : (c + 1) * 128].astype(jnp.float32)
                )
            top, total, outs = merged(stats, blocks, zi)
            zsend[k, zi] = jnp.concatenate(outs, axis=1).astype(jnp.bfloat16)
            if zi == 0:
                zsst[k] = jnp.where(st_lane < 64, top, total)
        for copy in z_copies(k, 1):
            copy.start()

        @pl.when(k > 0)
        def _():
            for copy in z_copies(k, 0):
                copy.start()

    @pl.loop(0, pairs + LAG)
    def _(it):
        @pl.when(it < pairs)
        def _():
            chunk(it)

        @pl.when(it >= LAG)
        def _():
            combine(it - LAG)

    for k in range(pairs):
        for zi in range(2):
            if (k, zi) != (0, 0):
                for copy in z_copies(k, zi):
                    copy.wait_recv()
    stats, blocks = [], []
    for k in range(pairs):
        for zi in range(2):
            own = (k, zi) == (0, 0)
            s = zsst[0] if own else zrst[k, zi]
            if zi == 1:
                s = pltpu.roll(s, 120, 1)
            stats.append(s)
            src = zsend[0, 0] if own else zrecv[k, zi]
            blocks.append(lambda c, src=src: src[:, c * 128 : (c + 1) * 128].astype(jnp.float32))
    _, total, outs = merged(stats, blocks, 0)
    tot_cols = [
        jnp.concatenate([total[:, 64 + c : 65 + c], total[:, 68 + c : 69 + c]], axis=0)
        for c in range(4)
    ]
    p_heads = []
    for h in range(2):
        one = outs[2 * h] / tot_cols[2 * h]
        two = outs[2 * h + 1] / tot_cols[2 * h + 1]
        p_heads.append(head_norm(one - lam[h] * two))
    hbuf[0] = jnp.concatenate(p_heads, axis=1).astype(jnp.bfloat16)
    for d in range(1, X):
        h_copy(hbuf, hs, hr, d).start()

    c_wo.wait()
    total_out = None
    for d in range(X):
        if d > 0:
            h_copy(hbuf, hs, hr, d).wait_recv()
            h_copy(dbuf, ds, dr, d).wait_recv()
        src = mod(tp + X - d, X)
        lhs = jnp.concatenate([hbuf[d], dbuf[d]], axis=0)
        part = jnp.dot(
            lhs, wo_v[pl.ds(pl.multiple_of(src * 256, 256), 256), :],
            preferred_element_type=jnp.float32,
        )
        total_out = part if total_out is None else total_out + part
    out_p[...] = total_out[:rows].astype(jnp.bfloat16)
    out_d[...] = total_out[rows : rows + 1].astype(jnp.bfloat16)

    for d in range(1, Z):
        q_z(d).wait_send()
    for o in range(Z):
        for e in range(1, Y):
            q_y(o, e).wait_send()
    for copy in (p_k, p_v, p_n):
        copy.wait_send()
    for k in range(pairs):
        for d in range(1, Y):
            for copy in y_copies(k, d):
                copy.wait_send()
        for zi in range(2):
            if (k, zi) != (0, 0):
                for copy in z_copies(k, zi):
                    copy.wait_send()
    for d in range(1, X):
        h_copy(hbuf, hs, hr, d).wait_send()
        h_copy(dbuf, ds, dr, d).wait_send()


def shards(Z, Y, X, *args):
    (x, xd, gain, wq, wk, wv, wo, hg, lam, pk, pv, ck, cv, lengths) = args
    D = x.shape[1]
    npos = pk.shape[0]
    slots = ck.shape[1]
    pairs = Z // 2
    bf, f32 = jnp.bfloat16, jnp.float32
    any_ = pl.BlockSpec(memory_space=pl.ANY)
    smem = pl.BlockSpec(memory_space=pltpu.SMEM)
    vmem = pl.BlockSpec(memory_space=pltpu.VMEM)
    V, S = pltpu.VMEM, pltpu.SemaphoreType.DMA
    out_cols = wo.shape[1]
    scratch = [
        V((16, D), bf), V((1, D), bf), V((1, D), f32), V((1, 128), f32),
        V((3, D, 256), bf), V(wo.shape, bf),
        V((2, 2 * npos, 128), bf), V((2, 2 * npos, 128), bf),
        V((2, 2 * npos + 128, 128), bf), V((2, 2 * npos + 128, 128), bf),
        V((2 * slots, 128), bf), V((2 * slots, 128), bf), V((2 * npos, 128), f32),
        V((16, 512), bf), V((16, 512), bf),
        V((Z, Y, 16, 256), bf),
        V((pairs, Y, 32, 512), bf), V((pairs, Y, 8, 128), f32),
        V((pairs, Y, 32, 512), bf), V((pairs, Y, 8, 128), f32),
        V((pairs, 2, 16, 512), bf), V((pairs, 8, 128), f32),
        V((pairs, 2, 16, 512), bf), V((pairs, 2, 8, 128), f32),
        V((X, 16, 256), bf), V((X, 16, 256), bf),
        S((12,)), S((3,)), S((3,)), S((Z,)), S((Z,)), S((Z, Y)), S((Z, Y)),
        S((pairs, Y)), S((pairs, Y)), S((pairs, Y)), S((pairs, Y)),
        S((pairs, 2)), S((pairs, 2)), S((pairs, 2)), S((pairs, 2)),
        S((X,)), S((X,)), S((X,)), S((X,)),
    ]
    return pl.pallas_call(
        functools.partial(kernel, Z, Y, X),
        out_shape=(
            jax.ShapeDtypeStruct((16, out_cols), bf),
            jax.ShapeDtypeStruct((1, out_cols), bf),
        ),
        in_specs=[any_] * 8 + [smem] + [any_] * 4 + [smem],
        out_specs=(vmem, vmem),
        scratch_shapes=scratch,
        compiler_params=pltpu.CompilerParams(collective_id=0, has_side_effects=True),
    )(
        x, xd, gain.reshape(1, D), wq, wk, wv, wo, hg.reshape(1, 128), lam,
        pk.reshape(2 * npos, 128), pv.reshape(2 * npos, 128),
        ck.reshape(2 * slots, 128), cv.reshape(2 * slots, 128), lengths,
    )


def solution(mesh):
    kv, X = mesh.shape["kv"], mesh.shape["tp"]
    Y = 4 if kv == 64 else 2
    Z = kv // (2 * Y)
    placed = (
        P("kv", None),
        P("kv", None),
        P(),
        P(None, "tp"),
        P(None, "tp"),
        P(None, "tp"),
        P(None, "tp"),
        P(),
        P("tp"),
        P("kv", "tp", None),
        P("kv", "tp", None),
        P("kv", None, "tp", None),
        P("kv", None, "tp", None),
        P("kv"),
    )
    return jax.shard_map(
        functools.partial(shards, Z, Y, X),
        mesh=mesh,
        in_specs=placed,
        out_specs=(P("kv", "tp"), P("kv", "tp")),
        check_vma=False,
    )
```

```python
import functools

import jax
import jax.numpy as jnp
from jax import lax
from jax.experimental import pallas as pl
from jax.experimental.pallas import tpu as pltpu
from jax.sharding import PartitionSpec as P

EPS = 1e-06
MESH = pl.DeviceIdType.MESH
NT = (((1,), (1,)), ((), ()))
LAG = 4


def kernel(
    Z, Y, X,
    x_hbm, xd_hbm, gain_hbm, wq_hbm, wk_hbm, wv_hbm, wo_hbm, hg_hbm, lam_hbm, pk_hbm, pv_hbm,
    ck_hbm, cv_hbm, len_hbm,
    out_ref,
    x_v, xd_v, gain_v, hg_v, w_v, wo_v, kraw, vraw, kd, vd, ck_v, cv_v, tmp,
    nkv, nkv_in, qbuf, ysend, yrecv, zsend, zrecv, hbuf, lam, length,
    lsem, ps, pr, qzs, qzr, qys, qyr, yds, ydr, zds, zdr, hs, hr,
):
    kv = lax.axis_index("kv")
    tp = lax.axis_index("tp")
    core = lax.rem(kv, 2)
    chip = lax.div(kv, 2)
    y = lax.rem(chip, Y)
    z = lax.div(chip, Y)
    rows = x_v.shape[0]
    npos = kraw.shape[1] // 2

    def dev(zz, yy):
        return ((zz * Y + yy) * 2 + core, tp)

    partner = (chip * 2 + 1 - core, tp)

    def xdev(xx):
        return (kv, xx)

    def mod(a, n):
        return lax.rem(a + n, n)

    barrier = pltpu.get_barrier_semaphore()
    for d in range(1, Z):
        pl.semaphore_signal(barrier, inc=1, device_id=dev(mod(z + d, Z), y), device_id_type=MESH)
    for d in range(1, Y):
        pl.semaphore_signal(barrier, inc=1, device_id=dev(z, mod(y + d, Y)), device_id_type=MESH)
    for d in range(1, X):
        pl.semaphore_signal(barrier, inc=1, device_id=xdev(mod(tp + d, X)), device_id_type=MESH)
    pl.semaphore_signal(barrier, inc=1, device_id=partner, device_id_type=MESH)

    local = []

    def fetch(src, dst):
        copy = pltpu.make_async_copy(src, dst, lsem.at[len(local)])
        copy.start()
        local.append(copy)
        return copy

    c_x = fetch(x_hbm, x_v)
    c_xd = fetch(xd_hbm, xd_v)
    c_gain = fetch(gain_hbm, gain_v)
    c_wq = fetch(wq_hbm, w_v.at[0])
    c_wk = fetch(wk_hbm, w_v.at[1])
    c_wv = fetch(wv_hbm, w_v.at[2])
    c_pk = fetch(pk_hbm, kraw.at[0])
    c_pv = fetch(pv_hbm, vraw.at[0])
    c_ck = fetch(ck_hbm, ck_v)
    c_cv = fetch(cv_hbm, cv_v)
    c_wo = fetch(wo_hbm, wo_v)
    c_hg = fetch(hg_hbm, hg_v)
    c_lam = fetch(lam_hbm, lam)
    c_len = fetch(len_hbm, length)

    def remote(src, dst, ssem, rsem, device):
        return pltpu.make_async_remote_copy(
            src_ref=src, dst_ref=dst, send_sem=ssem, recv_sem=rsem,
            device_id=device, device_id_type=MESH,
        )

    c_x.wait()
    c_xd.wait()
    c_gain.wait()
    gain = gain_v[...]

    def norm(v):
        v = v.astype(jnp.float32)
        return v * lax.rsqrt(jnp.mean(v * v, axis=-1, keepdims=True) + EPS) * gain

    normed_p = norm(x_v[...]).astype(jnp.bfloat16)
    normed_d = jnp.broadcast_to(norm(xd_v[...]), (16, x_v.shape[1])).astype(jnp.bfloat16)
    normed = jnp.concatenate([normed_p, normed_d], axis=0)

    def project(which):
        return jnp.dot(normed, w_v[which], preferred_element_type=jnp.float32).astype(jnp.bfloat16)

    c_wq.wait()
    queries = project(0) * jnp.bfloat16(0.125)
    qbuf[z, y] = queries[:rows]

    c_wk.wait()
    keys = project(1)
    c_wv.wait()
    values = project(2)
    nkv[...] = jnp.concatenate([keys[:rows], values[:rows]], axis=1)

    def split_heads(raw, which, out):
        tmp[...] = raw[which].astype(jnp.float32)
        for h in range(2):
            out[h, pl.ds(which * npos, npos), :] = tmp[
                pl.ds(h, npos, stride=2), :
            ].astype(jnp.bfloat16)

    c_pk.wait()
    split_heads(kraw, 0, kd)
    c_pv.wait()
    split_heads(vraw, 0, vd)

    pl.semaphore_wait(barrier, Z + Y + X - 2)

    def q_z(d):
        return remote(qbuf.at[z, y], qbuf.at[z, y], qzs, qzr.at[d], dev(mod(z + d, Z), y))

    def q_z_in(d):
        src = mod(z + Z - d, Z)
        return remote(qbuf.at[src, y], qbuf.at[src, y], qzs, qzr.at[d], dev(src, y))

    def q_y(o, e):
        zz = mod(z + o, Z)
        return remote(qbuf.at[zz, y], qbuf.at[zz, y], qys, qyr.at[o], dev(z, mod(y + e, Y)))

    def all_of(ref, ssem, rsem):
        return remote(ref, ref, ssem, rsem, partner)

    zorder = []
    for d in range(1, Z // 2 + 1):
        zorder.append(d)
        if Z - d not in zorder:
            zorder.append(Z - d)
    for d in reversed(zorder):
        q_z(d).start()
    for e in range(1, Y):
        q_y(0, e).start()

    p_k = remote(pk_hbm, kraw.at[1], ps.at[0], pr.at[0], partner)
    p_v = remote(pv_hbm, vraw.at[1], ps.at[1], pr.at[1], partner)
    p_n = remote(nkv, nkv_in, ps.at[2], pr.at[2], partner)
    p_n.start()
    p_k.start()
    p_v.start()

    def forward(d):
        q_z_in(d).wait_recv()
        for e in range(1, Y):
            q_y(Z - d, e).start()

    zeros = jnp.zeros((96, 128), jnp.bfloat16)
    p_n.wait_recv()
    for h in range(2):
        for out, base in ((kd, 0), (vd, 256)):
            cols = slice(base + h * 128, base + (h + 1) * 128)
            out[h, 2 * npos : 2 * npos + 16, :] = nkv[:, cols]
            out[h, 2 * npos + 16 : 2 * npos + 32, :] = nkv_in[:, cols]
            out[h, 2 * npos + 32 :, :] = zeros
    p_k.wait_recv()
    split_heads(kraw, 1, kd)
    p_v.wait_recv()
    split_heads(vraw, 1, vd)

    for d in zorder:
        forward(d)

    c_hg.wait()
    c_lam.wait()
    c_len.wait()
    head_gain = hg_v[...]

    def head_norm(a):
        return a * lax.rsqrt(jnp.mean(a * a, axis=-1, keepdims=True) + EPS) * head_gain

    def h_copy(part, d):
        at = pl.ds(16 * part, 16)
        return remote(hbuf.at[0, at], hbuf.at[d, at], hs, hr, xdev(mod(tp + d, X)))

    def decode():
        c_ck.wait()
        c_cv.wait()
        row_id = lax.broadcasted_iota(jnp.int32, (16, 128), 0)
        lane_id = lax.broadcasted_iota(jnp.int32, (16, 128), 1)
        first_head = (row_id & 3) < 2
        own_half = (lane_id >= 64) == ((row_id & 1) == 1)

        def by_head(m):
            m = m[rows:].astype(jnp.float32)
            return jnp.where(first_head, m[:, :128], m[:, 128:])

        dq = jnp.where(own_half, by_head(queries), 0.0)
        own_score = jnp.sum(dq * by_head(keys), axis=-1, keepdims=True)
        scores = lax.dot_general(
            dq.astype(jnp.bfloat16), ck_v[...], NT, preferred_element_type=jnp.float32
        )
        slots = scores.shape[1]
        s_row = lax.broadcasted_iota(jnp.int32, (16, slots), 0)
        s_col = lax.broadcasted_iota(jnp.int32, (16, slots), 1)
        head_ok = (s_col & 1) == ((s_row >> 1) & 1)
        scores = jnp.where(head_ok & (s_col < 2 * length[0]), scores, -jnp.inf)
        d_max = jnp.maximum(jnp.max(scores, axis=-1, keepdims=True), own_score)
        weights = jnp.exp(scores - d_max)
        own_weight = jnp.exp(own_score - d_max)
        d_tot = jnp.sum(weights, axis=-1, keepdims=True) + own_weight
        mixed = jnp.dot(weights.astype(jnp.bfloat16), cv_v[...], preferred_element_type=jnp.float32)
        mixed = mixed + own_weight.astype(jnp.bfloat16).astype(jnp.float32) * by_head(values)
        mixed = mixed / d_tot

        d_heads = []
        for h in range(2):
            att = mixed[2 * h : 2 * h + 1] - lam[h] * mixed[2 * h + 1 : 2 * h + 2]
            d_heads.append(jnp.broadcast_to(head_norm(att), (16, 128)))
        hbuf[0, 16:, :] = jnp.concatenate(d_heads, axis=1).astype(jnp.bfloat16)

        for d in range(1, X):
            h_copy(1, d).start()

    block = Y * 16
    st_lane = lax.broadcasted_iota(jnp.int32, (16, 128), 1)
    q_row = lax.rem(lax.broadcasted_iota(jnp.int32, (2 * block, 128), 0), block)
    q_lane = lax.broadcasted_iota(jnp.int32, (2 * block, 128), 1)
    q_off = lax.div(q_row, 16) * 32 + core * 16 + lax.rem(q_row, 16)
    key_core = jnp.where(q_lane < 16, core, 1 - core)
    key_pos = chip * 32 + key_core * 16 + lax.rem(q_lane, 16)
    lane1 = lax.broadcasted_iota(jnp.int32, (block, 128), 1)

    def offset(k):
        half = lax.div(k + 1, 2)
        return jnp.where(lax.rem(k, 2) == 1, half, lax.rem(Z - half, Z))

    def packed(stat):
        high = stat.astype(jnp.bfloat16).astype(jnp.float32)
        rest = stat - high
        middle = rest.astype(jnp.bfloat16).astype(jnp.float32)
        low = rest - middle
        return (high + pltpu.roll(middle, 16, 1) + pltpu.roll(low, 32, 1)).astype(jnp.bfloat16)

    def unpacked(tile):
        tile = tile.astype(jnp.float32)
        return tile + pltpu.roll(tile, 112, 1) + pltpu.roll(tile, 96, 1)

    def y_copy(k, d):
        to = mod(y + d, Y)
        return remote(ysend.at[k, to], yrecv.at[k, d - 1], yds, ydr.at[k], dev(z, to))

    def chunk(k):
        o = offset(k)
        zz = mod(z + o, Z)
        all_of(qbuf.at[zz, pl.ds(0, Y - 1)], qys, qyr.at[o]).wait_recv()
        q = qbuf[zz].reshape(block, 256)
        visible = (key_pos <= zz * (Y * 32) + q_off) & (q_lane < 32)
        stats = jnp.zeros((block, 128), jnp.float32)
        for h in range(2):
            qh = q[:, h * 128 : (h + 1) * 128]
            zero = jnp.zeros_like(qh)
            stacked = jnp.concatenate(
                [jnp.where(lane1 < 64, qh, zero), jnp.where(lane1 < 64, zero, qh)], axis=0
            )
            s = lax.dot_general(stacked, kd[h], NT, preferred_element_type=jnp.float32)
            s = jnp.concatenate(
                [s[:, : 2 * npos], jnp.where(visible, s[:, 2 * npos :], -jnp.inf)], axis=1
            )
            top = jnp.max(s, axis=-1, keepdims=True)
            w = jnp.exp(s - top)
            tot = jnp.sum(w, axis=-1, keepdims=True)
            acc = jnp.dot(
                w.astype(jnp.bfloat16), vd[h], preferred_element_type=jnp.float32
            ).astype(jnp.bfloat16)
            for m in range(2):
                combo = 2 * h + m
                of_map = slice(m * block, (m + 1) * block)
                stats = jnp.where(lane1 == combo, top[of_map], stats)
                stats = jnp.where(lane1 == combo + 64, tot[of_map], stats)
                for yy in range(Y):
                    base = m * block + yy * 16
                    ysend[k, yy, :, combo * 128 : (combo + 1) * 128] = acc[base : base + 16]
        stats = packed(stats)
        for yy in range(Y):
            ysend[k, yy, :, 512:] = stats[yy * 16 : yy * 16 + 16]
        for d in range(1, Y):
            y_copy(k, d).start()

    def merged(sources):
        stats = [unpacked(data[:, 512:]) for data in sources]
        top = functools.reduce(jnp.maximum, stats)
        scale = [jnp.exp(s - top) for s in stats]
        total = sum(pltpu.roll(f, 64, 1) * s for f, s in zip(scale, stats))
        outs = []
        for combo in range(4):
            acc = None
            for f, data in zip(scale, sources):
                term = f[:, combo : combo + 1] * data[
                    :, combo * 128 : (combo + 1) * 128
                ].astype(jnp.float32)
                acc = term if acc is None else acc + term
            outs.append(acc)
        return top, total, outs

    def z_copy(k):
        return remote(zsend.at[k], zrecv.at[k], zds, zdr, dev(mod(z + offset(k), Z), y))

    def combine(k):
        all_of(yrecv.at[k], yds, ydr.at[k]).wait_recv()
        top, total, outs = merged([ysend.at[k, y]] + [yrecv.at[k, i] for i in range(Y - 1)])
        for c in range(4):
            zsend[k, :, c * 128 : (c + 1) * 128] = outs[c].astype(jnp.bfloat16)
        totals = jnp.where((st_lane >= 64) & (st_lane < 68), total, 0.0)
        zsend[k, :, 512:] = packed(jnp.where(st_lane < 4, top, totals))

        @pl.when(k > 0)
        def _():
            z_copy(k).start()

    @pl.loop(0, Z + LAG)
    def _(it):
        @pl.when(it < Z)
        def _():
            chunk(it)

        @pl.when(it == Z - 1)
        def _():
            decode()

        @pl.when(it >= LAG)
        def _():
            combine(it - LAG)

    zall = all_of(zrecv.at[pl.ds(1, Z - 1)], zds, zdr)
    zall.wait_recv()
    _, total, outs = merged([zsend.at[0]] + [zrecv.at[k] for k in range(1, Z)])
    tot_cols = [total[:, 64 + c : 65 + c] for c in range(4)]
    p_heads = []
    for h in range(2):
        one = outs[2 * h] / tot_cols[2 * h]
        two = outs[2 * h + 1] / tot_cols[2 * h + 1]
        p_heads.append(head_norm(one - lam[h] * two))
    hbuf[0, :16, :] = jnp.concatenate(p_heads, axis=1).astype(jnp.bfloat16)
    for d in range(1, X):
        h_copy(0, d).start()

    c_wo.wait()

    def out_term(d):
        src = mod(tp + X - d, X)
        return jnp.dot(
            hbuf[d], wo_v[pl.ds(pl.multiple_of(src * 256, 256), 256), :],
            preferred_element_type=jnp.float32,
        )

    total_out = out_term(0)
    if X > 1:
        all_of(hbuf.at[pl.ds(1, X - 1)], hs, hr).wait_recv()
    for d in range(1, X):
        total_out = total_out + out_term(d)
    out_ref[...] = total_out.astype(jnp.bfloat16)

    all_of(qbuf.at[pl.ds(0, Z - 1), 0], qzs, qzr.at[0]).wait_send()
    all_of(qbuf.at[:, pl.ds(0, Y - 1)], qys, qyr.at[0]).wait_send()
    for copy in (p_k, p_v, p_n):
        copy.wait_send()
    all_of(ysend.at[:, pl.ds(0, Y - 1)], yds, ydr.at[0]).wait_send()
    zall.wait_send()
    if X > 1:
        all_of(hbuf.at[pl.ds(1, X - 1)], hs, hr).wait_send()


def shards(Z, Y, X, *args):
    (x, xd, gain, wq, wk, wv, wo, hg, lam, pk, pv, ck, cv, lengths) = args
    D = x.shape[1]
    npos = pk.shape[0]
    slots = ck.shape[1]
    bf, f32 = jnp.bfloat16, jnp.float32
    any_ = pl.BlockSpec(memory_space=pl.ANY)
    vmem = pl.BlockSpec(memory_space=pltpu.VMEM)
    V, S = pltpu.VMEM, pltpu.SemaphoreType.DMA
    out_cols = wo.shape[1]
    scratch = [
        V((16, D), bf), V((1, D), bf), V((1, D), f32), V((1, 128), f32),
        V((3, D, 256), bf), V(wo.shape, bf),
        V((2, 2 * npos, 128), bf), V((2, 2 * npos, 128), bf),
        V((2, 2 * npos + 128, 128), bf), V((2, 2 * npos + 128, 128), bf),
        V((2 * slots, 128), bf), V((2 * slots, 128), bf), V((2 * npos, 128), f32),
        V((16, 512), bf), V((16, 512), bf),
        V((Z, Y, 16, 256), bf),
        V((Z, Y, 16, 640), bf), V((Z, Y - 1, 16, 640), bf),
        V((Z, 16, 640), bf), V((Z, 16, 640), bf), V((X, 32, 256), bf),
        pltpu.SMEM((2,), f32), pltpu.SMEM((1,), jnp.int32),
        S((14,)), S((3,)), S((3,)), S, S((Z,)), S, S((Z,)), S, S((Z,)), S, S, S, S,
    ]
    out = pl.pallas_call(
        functools.partial(kernel, Z, Y, X),
        out_shape=jax.ShapeDtypeStruct((32, out_cols), bf),
        in_specs=[any_] * 14,
        out_specs=vmem,
        scratch_shapes=scratch,
        compiler_params=pltpu.CompilerParams(collective_id=0, has_side_effects=True),
    )(
        x, xd, gain.reshape(1, D), wq, wk, wv, wo, hg.reshape(1, 128), lam,
        pk.reshape(2 * npos, 128), pv.reshape(2 * npos, 128),
        ck.reshape(2 * slots, 128), cv.reshape(2 * slots, 128), lengths,
    )
    return out[:16], out[16:17]


def solution(mesh):
    kv, X = mesh.shape["kv"], mesh.shape["tp"]
    Y = 4
    Z = kv // (2 * Y)
    placed = (
        P("kv", None),
        P("kv", None),
        P(),
        P(None, "tp"),
        P(None, "tp"),
        P(None, "tp"),
        P(None, "tp"),
        P(),
        P("tp"),
        P("kv", "tp", None),
        P("kv", "tp", None),
        P("kv", None, "tp", None),
        P("kv", None, "tp", None),
        P("kv"),
    )
    return jax.shard_map(
        functools.partial(shards, Z, Y, X),
        mesh=mesh,
        in_specs=placed,
        out_specs=(P("kv", "tp"), P("kv", "tp")),
        check_vma=False,
    )
```

```python
import functools

import jax
import jax.numpy as jnp
from jax import lax
from jax.experimental import pallas as pl
from jax.experimental.pallas import tpu as pltpu
from jax.sharding import PartitionSpec as P

EPS = 1e-06
MESH = pl.DeviceIdType.MESH
NT = (((1,), (1,)), ((), ()))
LAG = 4


def kernel(
    Z, Y, X,
    x_hbm, xd_hbm, gain_hbm, wq_hbm, wk_hbm, wv_hbm, wo_hbm, hg_hbm, lam_hbm, pk_hbm, pv_hbm,
    ck_hbm, cv_hbm, len_hbm,
    out_ref,
    x_v, xd_v, gain_v, hg_v, w_v, wo_v, kraw, vraw, kd, vd, ck_v, cv_v, tmp,
    nkv, nkv_in, qbuf, ysend, yrecv, zsend, zrecv, hbuf, lam, length,
    lsem, ps, pr, qzs, qzr, qys, qyr, yds, ydr, zds, zdr, hs, hr,
):
    kv = lax.axis_index("kv")
    tp = lax.axis_index("tp")
    core = lax.rem(kv, 2)
    chip = lax.div(kv, 2)
    y = lax.rem(chip, Y)
    z = lax.div(chip, Y)
    rows = x_v.shape[0]
    npos = kraw.shape[1] // 2

    def dev(zz, yy):
        return ((zz * Y + yy) * 2 + core, tp)

    partner = (chip * 2 + 1 - core, tp)

    def xdev(xx):
        return (kv, xx)

    def mod(a, n):
        return lax.rem(a + n, n)

    barrier = pltpu.get_barrier_semaphore()
    for d in range(1, Z):
        pl.semaphore_signal(barrier, inc=1, device_id=dev(mod(z + d, Z), y), device_id_type=MESH)
    for d in range(1, Y):
        pl.semaphore_signal(barrier, inc=1, device_id=dev(z, mod(y + d, Y)), device_id_type=MESH)
    for d in range(1, X):
        pl.semaphore_signal(barrier, inc=1, device_id=xdev(mod(tp + d, X)), device_id_type=MESH)
    pl.semaphore_signal(barrier, inc=1, device_id=partner, device_id_type=MESH)

    local = []

    def fetch(src, dst):
        copy = pltpu.make_async_copy(src, dst, lsem.at[len(local)])
        copy.start()
        local.append(copy)
        return copy

    c_x = fetch(x_hbm, x_v)
    c_xd = fetch(xd_hbm, xd_v)
    c_gain = fetch(gain_hbm, gain_v)
    c_wq = fetch(wq_hbm, w_v.at[0])
    c_wk = fetch(wk_hbm, w_v.at[1])
    c_wv = fetch(wv_hbm, w_v.at[2])
    c_pk = fetch(pk_hbm, kraw.at[0])
    c_pv = fetch(pv_hbm, vraw.at[0])
    c_ck = fetch(ck_hbm, ck_v)
    c_cv = fetch(cv_hbm, cv_v)
    c_wo = fetch(wo_hbm, wo_v)
    c_hg = fetch(hg_hbm, hg_v)
    c_lam = fetch(lam_hbm, lam)
    c_len = fetch(len_hbm, length)

    def remote(src, dst, ssem, rsem, device):
        return pltpu.make_async_remote_copy(
            src_ref=src, dst_ref=dst, send_sem=ssem, recv_sem=rsem,
            device_id=device, device_id_type=MESH,
        )

    c_x.wait()
    c_xd.wait()
    c_gain.wait()
    gain = gain_v[...]

    def norm(v):
        v = v.astype(jnp.float32)
        return v * lax.rsqrt(jnp.mean(v * v, axis=-1, keepdims=True) + EPS) * gain

    normed_p = norm(x_v[...]).astype(jnp.bfloat16)
    normed_d = jnp.broadcast_to(norm(xd_v[...]), (16, x_v.shape[1])).astype(jnp.bfloat16)
    normed = jnp.concatenate([normed_p, normed_d], axis=0)

    def project(which):
        return jnp.dot(normed, w_v[which], preferred_element_type=jnp.float32).astype(jnp.bfloat16)

    c_wq.wait()
    queries = project(0) * jnp.bfloat16(0.125)
    qbuf[z, y] = queries[:rows]

    c_wk.wait()
    keys = project(1)
    c_wv.wait()
    values = project(2)
    nkv[...] = jnp.concatenate([keys[:rows], values[:rows]], axis=1)

    def split_heads(raw, which, out):
        tmp[...] = raw[which].astype(jnp.float32)
        for h in range(2):
            out[h, pl.ds(which * npos, npos), :] = tmp[
                pl.ds(h, npos, stride=2), :
            ].astype(jnp.bfloat16)

    c_pk.wait()
    split_heads(kraw, 0, kd)
    c_pv.wait()
    split_heads(vraw, 0, vd)

    pl.semaphore_wait(barrier, Z + Y + X - 2)

    def q_z(d):
        return remote(qbuf.at[z, y], qbuf.at[z, y], qzs, qzr.at[d], dev(mod(z + d, Z), y))

    def q_z_in(d):
        src = mod(z + Z - d, Z)
        return remote(qbuf.at[src, y], qbuf.at[src, y], qzs, qzr.at[d], dev(src, y))

    def q_y(o, e):
        zz = mod(z + o, Z)
        return remote(qbuf.at[zz, y], qbuf.at[zz, y], qys, qyr.at[o], dev(z, mod(y + e, Y)))

    def all_of(ref, ssem, rsem):
        return remote(ref, ref, ssem, rsem, partner)

    zorder = []
    for d in range(1, Z // 2 + 1):
        zorder.append(d)
        if Z - d not in zorder:
            zorder.append(Z - d)
    for d in reversed(zorder):
        q_z(d).start()
    for e in range(1, Y):
        q_y(0, e).start()

    p_k = remote(pk_hbm, kraw.at[1], ps.at[0], pr.at[0], partner)
    p_v = remote(pv_hbm, vraw.at[1], ps.at[1], pr.at[1], partner)
    p_n = remote(nkv, nkv_in, ps.at[2], pr.at[2], partner)
    p_n.start()
    p_k.start()
    p_v.start()

    def forward(d):
        q_z_in(d).wait_recv()
        for e in range(1, Y):
            q_y(Z - d, e).start()

    zeros = jnp.zeros((96, 128), jnp.bfloat16)
    p_n.wait_recv()
    for h in range(2):
        for out, base in ((kd, 0), (vd, 256)):
            cols = slice(base + h * 128, base + (h + 1) * 128)
            out[h, 2 * npos : 2 * npos + 16, :] = nkv[:, cols]
            out[h, 2 * npos + 16 : 2 * npos + 32, :] = nkv_in[:, cols]
            out[h, 2 * npos + 32 :, :] = zeros
    p_k.wait_recv()
    split_heads(kraw, 1, kd)
    p_v.wait_recv()
    split_heads(vraw, 1, vd)

    for d in zorder:
        forward(d)

    c_hg.wait()
    c_lam.wait()
    c_len.wait()
    head_gain = hg_v[...]

    def head_norm(a):
        return a * lax.rsqrt(jnp.mean(a * a, axis=-1, keepdims=True) + EPS) * head_gain

    def h_copy(part, d):
        at = pl.ds(16 * part, 16)
        return remote(hbuf.at[0, at], hbuf.at[d, at], hs, hr, xdev(mod(tp + d, X)))

    def decode():
        c_ck.wait()
        c_cv.wait()
        row_id = lax.broadcasted_iota(jnp.int32, (16, 128), 0)
        lane_id = lax.broadcasted_iota(jnp.int32, (16, 128), 1)
        first_head = (row_id & 3) < 2
        own_half = (lane_id >= 64) == ((row_id & 1) == 1)

        def by_head(m):
            m = m[rows:].astype(jnp.float32)
            return jnp.where(first_head, m[:, :128], m[:, 128:])

        dq = jnp.where(own_half, by_head(queries), 0.0)
        own_score = jnp.sum(dq * by_head(keys), axis=-1, keepdims=True)
        scores = lax.dot_general(
            dq.astype(jnp.bfloat16), ck_v[...], NT, preferred_element_type=jnp.float32
        )
        slots = scores.shape[1]
        s_row = lax.broadcasted_iota(jnp.int32, (16, slots), 0)
        s_col = lax.broadcasted_iota(jnp.int32, (16, slots), 1)
        head_ok = (s_col & 1) == ((s_row >> 1) & 1)
        scores = jnp.where(head_ok & (s_col < 2 * length[0]), scores, -jnp.inf)
        d_max = jnp.maximum(jnp.max(scores, axis=-1, keepdims=True), own_score)
        weights = jnp.exp(scores - d_max)
        own_weight = jnp.exp(own_score - d_max)
        d_tot = jnp.sum(weights, axis=-1, keepdims=True) + own_weight
        mixed = jnp.dot(weights.astype(jnp.bfloat16), cv_v[...], preferred_element_type=jnp.float32)
        mixed = mixed + own_weight.astype(jnp.bfloat16).astype(jnp.float32) * by_head(values)
        mixed = mixed / d_tot

        d_heads = []
        for h in range(2):
            att = mixed[2 * h : 2 * h + 1] - lam[h] * mixed[2 * h + 1 : 2 * h + 2]
            d_heads.append(jnp.broadcast_to(head_norm(att), (16, 128)))
        hbuf[0, 16:, :] = jnp.concatenate(d_heads, axis=1).astype(jnp.bfloat16)

        for d in range(1, X):
            h_copy(1, d).start()

    block = Y * 16
    st_lane = lax.broadcasted_iota(jnp.int32, (16, 128), 1)
    q_row = lax.broadcasted_iota(jnp.int32, (block, 128), 0)
    q_lane = lax.broadcasted_iota(jnp.int32, (block, 128), 1)
    q_off = lax.div(q_row, 16) * 32 + core * 16 + lax.rem(q_row, 16)
    key_core = jnp.where(q_lane < 16, core, 1 - core)
    key_pos = chip * 32 + key_core * 16 + lax.rem(q_lane, 16)
    lane1 = lax.broadcasted_iota(jnp.int32, (2 * block, 128), 1)

    def offset(k):
        half = lax.div(k + 1, 2)
        return jnp.where(lax.rem(k, 2) == 1, half, lax.rem(Z - half, Z))

    def packed(stat):
        high = stat.astype(jnp.bfloat16).astype(jnp.float32)
        rest = stat - high
        middle = rest.astype(jnp.bfloat16).astype(jnp.float32)
        low = rest - middle
        return (high + pltpu.roll(middle, 16, 1) + pltpu.roll(low, 32, 1)).astype(jnp.bfloat16)

    def unpacked(tile):
        tile = tile.astype(jnp.float32)
        return tile + pltpu.roll(tile, 112, 1) + pltpu.roll(tile, 96, 1)

    def y_copy(k, d):
        to = mod(y + d, Y)
        return remote(ysend.at[k + 1, to], yrecv.at[k, d - 1], yds, ydr.at[k], dev(z, to))

    def blocks_of(it):
        return [2 * it - 1, 2 * it]

    def chunk(it):
        ks = blocks_of(it)
        where_from = [mod(z + offset(jnp.clip(k, 0, Z - 1)), Z) for k in ks]
        for k, zz in zip(ks, where_from):
            @pl.when((k >= 0) & (k < Z))
            def _(k=k, zz=zz):
                all_of(qbuf.at[zz, pl.ds(0, Y - 1)], qys, qyr.at[offset(k)]).wait_recv()

        q = jnp.concatenate([qbuf[zz].reshape(block, 256) for zz in where_from], axis=0)
        visible = jnp.concatenate(
            [(key_pos <= zz * (Y * 32) + q_off) & (q_lane < 32) for zz in where_from] * 2, axis=0
        )
        count = 2 * block
        stats = jnp.zeros((count, 128), jnp.float32)
        for h in range(2):
            qh = q[:, h * 128 : (h + 1) * 128]
            zero = jnp.zeros_like(qh)
            stacked = jnp.concatenate(
                [jnp.where(lane1 < 64, qh, zero), jnp.where(lane1 < 64, zero, qh)], axis=0
            )
            s = lax.dot_general(stacked, kd[h], NT, preferred_element_type=jnp.float32)
            s = jnp.concatenate(
                [s[:, : 2 * npos], jnp.where(visible, s[:, 2 * npos :], -jnp.inf)], axis=1
            )
            top = jnp.max(s, axis=-1, keepdims=True)
            w = jnp.exp(s - top)
            tot = jnp.sum(w, axis=-1, keepdims=True)
            acc = jnp.dot(
                w.astype(jnp.bfloat16), vd[h], preferred_element_type=jnp.float32
            ).astype(jnp.bfloat16)
            for m in range(2):
                combo = 2 * h + m
                of_map = slice(m * count, (m + 1) * count)
                stats = jnp.where(lane1 == combo, top[of_map], stats)
                stats = jnp.where(lane1 == combo + 64, tot[of_map], stats)
                for b, k in enumerate(ks):
                    for yy in range(Y):
                        base = m * count + b * block + yy * 16
                        ysend[k + 1, yy, :, combo * 128 : (combo + 1) * 128] = acc[base : base + 16]
        stats = packed(stats)
        for b, k in enumerate(ks):
            for yy in range(Y):
                base = b * block + yy * 16
                ysend[k + 1, yy, :, 512:] = stats[base : base + 16]

            @pl.when((k >= 0) & (k < Z))
            def _(k=k):
                for d in range(1, Y):
                    y_copy(k, d).start()

    def merged(sources):
        stats = [unpacked(data[:, 512:]) for data in sources]
        top = functools.reduce(jnp.maximum, stats)
        scale = [jnp.exp(s - top) for s in stats]
        total = sum(pltpu.roll(f, 64, 1) * s for f, s in zip(scale, stats))
        outs = []
        for combo in range(4):
            acc = None
            for f, data in zip(scale, sources):
                term = f[:, combo : combo + 1] * data[
                    :, combo * 128 : (combo + 1) * 128
                ].astype(jnp.float32)
                acc = term if acc is None else acc + term
            outs.append(acc)
        return top, total, outs

    def z_copy(k):
        return remote(zsend.at[k], zrecv.at[k], zds, zdr, dev(mod(z + offset(k), Z), y))

    def combine(k):
        all_of(yrecv.at[k], yds, ydr.at[k]).wait_recv()
        top, total, outs = merged([ysend.at[k + 1, y]] + [yrecv.at[k, i] for i in range(Y - 1)])
        for c in range(4):
            zsend[k, :, c * 128 : (c + 1) * 128] = outs[c].astype(jnp.bfloat16)
        totals = jnp.where((st_lane >= 64) & (st_lane < 68), total, 0.0)
        zsend[k, :, 512:] = packed(jnp.where(st_lane < 4, top, totals))

        @pl.when(k > 0)
        def _():
            z_copy(k).start()

    steps = Z // 2 + 1

    @pl.loop(0, steps + LAG)
    def _(it):
        @pl.when(it == 1)
        def _():
            decode()

        @pl.when(it < steps)
        def _():
            chunk(it)

        for k in blocks_of(it - LAG):
            @pl.when((k >= 0) & (k < Z))
            def _(k=k):
                combine(k)

    zall = all_of(zrecv.at[pl.ds(1, Z - 1)], zds, zdr)
    zall.wait_recv()
    _, total, outs = merged([zsend.at[0]] + [zrecv.at[k] for k in range(1, Z)])
    tot_cols = [total[:, 64 + c : 65 + c] for c in range(4)]
    p_heads = []
    for h in range(2):
        one = outs[2 * h] / tot_cols[2 * h]
        two = outs[2 * h + 1] / tot_cols[2 * h + 1]
        p_heads.append(head_norm(one - lam[h] * two))
    hbuf[0, :16, :] = jnp.concatenate(p_heads, axis=1).astype(jnp.bfloat16)
    for d in range(1, X):
        h_copy(0, d).start()

    c_wo.wait()

    def out_term(d):
        src = mod(tp + X - d, X)
        return jnp.dot(
            hbuf[d], wo_v[pl.ds(pl.multiple_of(src * 256, 256), 256), :],
            preferred_element_type=jnp.float32,
        )

    total_out = out_term(0)
    if X > 1:
        all_of(hbuf.at[pl.ds(1, X - 1)], hs, hr).wait_recv()
    for d in range(1, X):
        total_out = total_out + out_term(d)
    out_ref[...] = total_out.astype(jnp.bfloat16)

    all_of(qbuf.at[pl.ds(0, Z - 1), 0], qzs, qzr.at[0]).wait_send()
    all_of(qbuf.at[:, pl.ds(0, Y - 1)], qys, qyr.at[0]).wait_send()
    for copy in (p_k, p_v, p_n):
        copy.wait_send()
    all_of(ysend.at[pl.ds(1, Z), pl.ds(0, Y - 1)], yds, ydr.at[0]).wait_send()
    zall.wait_send()
    if X > 1:
        all_of(hbuf.at[pl.ds(1, X - 1)], hs, hr).wait_send()


def shards(Z, Y, X, *args):
    (x, xd, gain, wq, wk, wv, wo, hg, lam, pk, pv, ck, cv, lengths) = args
    D = x.shape[1]
    npos = pk.shape[0]
    slots = ck.shape[1]
    bf, f32 = jnp.bfloat16, jnp.float32
    any_ = pl.BlockSpec(memory_space=pl.ANY)
    vmem = pl.BlockSpec(memory_space=pltpu.VMEM)
    V, S = pltpu.VMEM, pltpu.SemaphoreType.DMA
    out_cols = wo.shape[1]
    scratch = [
        V((16, D), bf), V((1, D), bf), V((1, D), f32), V((1, 128), f32),
        V((3, D, 256), bf), V(wo.shape, bf),
        V((2, 2 * npos, 128), bf), V((2, 2 * npos, 128), bf),
        V((2, 2 * npos + 128, 128), bf), V((2, 2 * npos + 128, 128), bf),
        V((2 * slots, 128), bf), V((2 * slots, 128), bf), V((2 * npos, 128), f32),
        V((16, 512), bf), V((16, 512), bf),
        V((Z, Y, 16, 256), bf),
        V((Z + 2, Y, 16, 640), bf), V((Z, Y - 1, 16, 640), bf),
        V((Z, 16, 640), bf), V((Z, 16, 640), bf), V((X, 32, 256), bf),
        pltpu.SMEM((2,), f32), pltpu.SMEM((1,), jnp.int32),
        S((14,)), S((3,)), S((3,)), S, S((Z,)), S, S((Z,)), S, S((Z,)), S, S, S, S,
    ]
    out = pl.pallas_call(
        functools.partial(kernel, Z, Y, X),
        out_shape=jax.ShapeDtypeStruct((32, out_cols), bf),
        in_specs=[any_] * 14,
        out_specs=vmem,
        scratch_shapes=scratch,
        compiler_params=pltpu.CompilerParams(collective_id=0, has_side_effects=True),
    )(
        x, xd, gain.reshape(1, D), wq, wk, wv, wo, hg.reshape(1, 128), lam,
        pk.reshape(2 * npos, 128), pv.reshape(2 * npos, 128),
        ck.reshape(2 * slots, 128), cv.reshape(2 * slots, 128), lengths,
    )
    return out[:16], out[16:17]


def solution(mesh):
    kv, X = mesh.shape["kv"], mesh.shape["tp"]
    Y = 4
    Z = kv // (2 * Y)
    placed = (
        P("kv", None),
        P("kv", None),
        P(),
        P(None, "tp"),
        P(None, "tp"),
        P(None, "tp"),
        P(None, "tp"),
        P(),
        P("tp"),
        P("kv", "tp", None),
        P("kv", "tp", None),
        P("kv", None, "tp", None),
        P("kv", None, "tp", None),
        P("kv"),
    )
    return jax.shard_map(
        functools.partial(shards, Z, Y, X),
        mesh=mesh,
        in_specs=placed,
        out_specs=(P("kv", "tp"), P("kv", "tp")),
        check_vma=False,
    )
```
